32 devices in a mesh: sp: 8 (over z, x), tp: 4 (over y, core).
Axes of the slice: x: 2, y: 2, z: 4, core: 2. Of those that a mesh axis runs over, the one named last changes fastest.
Arguments:
- layer_input: bfloat16 [1024, 2048], P('sp', 'tp'), may hold values from -6 to 6
- cotangent: bfloat16 [1024, 2048], P('sp', 'tp'), may hold values from -6 to 6
- routes: int32 [1024, 2], P('sp'), may hold values from 0 to 7, all different within a row; in each aligned block of 128 rows (0 to 127, 128 to 255, ...) at most 48 rows name the same one
- route_weight: float32 [1024, 2], P('sp'), may hold values from 0.1 to 0.6
- gate_weight: bfloat16 [8, 2048, 1024], P('sp', None, 'tp'), may hold values from -0.125 to 0.125
- up_weight: bfloat16 [8, 2048, 1024], P('sp', None, 'tp'), may hold values from -0.125 to 0.125
- down_weight: bfloat16 [8, 1024, 2048], P('sp', 'tp'), may hold values from -0.1875 to 0.1875
- heads_value: bfloat16 [1024, 2048], P('sp', 'tp'), may hold values from -6 to 6
- output_gate: bfloat16 [1024, 2048], P('sp', 'tp'), may hold values from -8 to 8
- mixer_saved: bfloat16 [1024, 2048], P('sp', 'tp'), may hold values from -6 to 6
- proj_weight: bfloat16 [2048, 2048], P(None, 'tp'), may hold values from -0.125 to 0.125
- state_write: bfloat16 [1024, 512], P('sp', 'tp'), may hold values from -0.5 to 0.5
- state_read: bfloat16 [1024, 512], P('sp', 'tp'), may hold values from -0.5 to 0.5
- decay_rate: float32 [1024, 32], P('sp', 'tp'), may hold values from 0 to 1.1, as said below
Outputs:
- gate_grad: bfloat16 [8, 2048, 1024], P('sp', None, 'tp')
- up_grad: bfloat16 [8, 2048, 1024], P('sp', None, 'tp')
- down_grad: bfloat16 [8, 1024, 2048], P('sp', 'tp')
- proj_grad: float32 [2048, 2048], P('sp', 'tp')
- value_grad: bfloat16 [1024, 2048], P('sp', 'tp')
- write_gradient: bfloat16 [1024, 512], P('sp', 'tp')
- read_gradient: bfloat16 [1024, 512], P('sp', 'tp')
- outgate_grad: bfloat16 [1024, 2048], P('sp', 'tp')
The draws below stay inside these ranges and needn't reach their ends.
Inputs may be any that keep to these rules, and one draw needn't show every extreme that they name: `routes`: each row names 2 different experts; within the rows of one aligned block of 128 tokens no expert is named by more than 48 rows, a bound that some block reaches. `decay_rate`: positive log-decays.
All inputs are finite; a program needn't handle non-finite values.
Results may differ from the reference program's by a relative error of at most 0.017.
Values may be sent and summed in bfloat16 or wider, within the bound.
A program may use at most 128 MiB of HBM per device.

```python
import math
import jax
import jax.numpy as jnp
import numpy as np
from jax import lax

D = 2048
BLENDER_CHANNEL = 32
HEAD_DIM = 64
GROUPS = 4
STATE = 128
EXP_HIDDEN = 1024
TOPK = 2
TOK_DEV = 128
SERIES_ENTRIES = 1024
EXPERTS = 8
CAP = 48
SSD_W = 2048
N_SP = 8
N_TP = 4


def draw_decay_rate(key, part):
    address_rows = jax.random.split(jax.random.fold_in(key, 11), 5)
    share = 0.5
    fast_heads = jax.random.uniform(address_rows[0], (BLENDER_CHANNEL,), jnp.float32) < share
    random_noise = jax.random.uniform(address_rows[1], (SERIES_ENTRIES, BLENDER_CHANNEL), jnp.float32, 0.5, 1.5)
    block_multiplier = jax.random.uniform(address_rows[2], (SERIES_ENTRIES // TOK_DEV, 1, 1), jnp.float32, 0.5, 1.5)
    block_multiplier = jnp.broadcast_to(block_multiplier, (SERIES_ENTRIES // TOK_DEV, TOK_DEV, 1)).reshape(SERIES_ENTRIES, 1)
    baseline_rate = jnp.where(fast_heads, 0.03, 0.5 / SERIES_ENTRIES)[None, :]
    interval_starts = jax.random.randint(address_rows[3], (2, BLENDER_CHANNEL), 0, SERIES_ENTRIES)
    interval_spans = jax.random.uniform(address_rows[4], (2, BLENDER_CHANNEL), jnp.float32, 0.22, 0.5)
    entry_indices = jnp.arange(SERIES_ENTRIES, dtype=jnp.int32)[:, None]
    pulse_clusters = jnp.where(entry_indices == interval_starts[0][None, :], interval_spans[0][None, :], 0.0)
    pulse_clusters = pulse_clusters + jnp.where(entry_indices == interval_starts[1][None, :], interval_spans[1][None, :], 0.0)
    pulse_clusters = jnp.where(fast_heads[None, :], 0.0, pulse_clusters)
    return (baseline_rate * random_noise * block_multiplier + pulse_clusters).astype(jnp.float32)


def raised(result, rng, source, target, shards_of, factor):
    def block_of(dim):
        return (jnp.arange(result.shape[dim]) // (result.shape[dim] // shards_of)).reshape((-1,) + (1,) * (result.ndim - 1 - dim))

    first = jax.random.permutation(rng, shards_of)[block_of(target)]
    second = (block_of(target) + shards_of // 2) % shards_of
    return jnp.where((block_of(source) == first) | (block_of(source) == second), factor * result, result)


def steps_of(rng, shape, cuts, least, high):
    def one(dim, blocks):
        heights = jax.random.uniform(jax.random.fold_in(jax.random.fold_in(rng, 6), dim), (blocks,), jnp.float32, least / len(cuts), high / len(cuts))
        return jnp.repeat(jnp.exp(heights), shape[dim] // blocks).reshape((-1,) + (1,) * (len(shape) - dim - 1))

    gain = one(*cuts[0])
    for cut in cuts[1:]:
        gain = gain * one(*cut)
    return gain


def deal_out(rng, own, number, rows, count, top, reach, skew):
    order = jax.random.permutation(rng, count)
    heavy_load, usual = shares(count, rows * top, reach, skew, True), shares(count, rows * top, reach, skew, False)
    places = jnp.arange(count)

    def named(tallies, offset_by):
        used = int((tallies > 0).sum())
        fixed = max(1, used // 4)
        moved = fixed + (places - fixed + offset_by * (used - fixed)) % max(1, count - fixed)
        return jnp.zeros((count,), jnp.int32).at[order[jnp.where(places < fixed, places, moved)]].set(jnp.asarray(tallies, jnp.int32))

    tallies = jnp.where(number % 4 == 0, named(heavy_load, number // 4), named(usual, number - number // 4 - 1))
    mixed = jax.random.permutation(jax.random.fold_in(own, 3), count)
    donor, taker = mixed[0:count // 2 * 2:2], mixed[1:count // 2 * 2:2]
    room = jnp.minimum(tallies[donor] - 1, reach - tallies[taker]) // 2
    room = jnp.where((donor == order[0]) | (taker == order[0]) | (tallies[taker] == 0), 0, jnp.maximum(room, 0))
    moved = jax.random.randint(jax.random.fold_in(own, 4), (count // 2,), 0, 1 << 20) % (room + 1)
    tallies = tallies.at[donor].add(-moved).at[taker].add(moved)
    items = jnp.searchsorted(jnp.cumsum(tallies), jnp.arange(rows * top), side="right").astype(jnp.int32)
    grid = items.reshape(top, rows).T
    grid = grid[jax.random.permutation(jax.random.fold_in(own, 1), rows)]
    offset_by = jax.random.randint(jax.random.fold_in(own, 2), (rows, 1), 0, top)
    return jnp.take_along_axis(grid, (jnp.arange(top)[None, :] + offset_by) % top, axis=1)


def shares(number_of, total, most, lean, full):
    weights = [(1 << 20) // math.isqrt(standing ** lean) + 1 for standing in range(1, number_of + 1)]
    largest = most if full else min(most, max(-(-total // number_of), total * weights[0] // sum(weights)))
    least = 1 if total - largest >= number_of - 1 else 0
    counts, surplus = [largest] + [least] * (number_of - 1), total - largest - least * (number_of - 1)
    while surplus > 0:
        free = [i for i in range(1, number_of) if counts[i] < largest] or [i for i in range(1, number_of) if counts[i] < most]
        pool, left = sum([weights[i] for i in free]), surplus
        for i in free:
            addition = min(most - counts[i], max(1, left * weights[i] // pool), surplus)
            counts[i] = counts[i] + addition
            surplus = surplus - addition
    return np.array(counts)


def gaussian(key, shape, deviation, limit, cuts=(), held_as=jnp.bfloat16):
    drawn = deviation * jax.random.normal(key, shape, jnp.float32)
    if cuts:
        drawn = drawn * steps_of(key, shape, cuts, -0.22, 0.18)
    return jnp.clip(drawn, -limit, limit).astype(held_as)


def heavy_noise(own_key, extent, deviation, reach, shards, heavy, held_as=jnp.bfloat16):
    array = deviation * jax.random.normal(own_key, extent, jnp.float32)
    if shards:
        array = array * steps_of(own_key, extent, shards, -0.22, 0.18)
    return jnp.clip(raised(array, jax.random.fold_in(own_key, 3), *heavy), -reach, reach).astype(held_as)


def setup_inputs(seed: int = 0) -> dict:
    seeds = jax.random.split(jax.random.key(seed), 15)
    layer_input = gaussian(seeds[0], (SERIES_ENTRIES, D), 1.0, 6.0, ((0, 8), (1, 4)))
    cotangent = heavy_noise(seeds[1], (SERIES_ENTRIES, D), 1.0, 6.0, ((0, 8), (1, 4)), (0, 1, 8, 2.0))
    routes_keys = jax.random.split(jax.random.fold_in(seeds[2], 1), SERIES_ENTRIES // TOK_DEV)
    routes_turns = jax.random.permutation(jax.random.fold_in(seeds[2], 3), SERIES_ENTRIES // TOK_DEV)
    routes = jax.vmap(lambda own, number: deal_out(jax.random.fold_in(seeds[2], 2), own, number, TOK_DEV, EXPERTS, TOPK, CAP, 1))(routes_keys, routes_turns).reshape((SERIES_ENTRIES, TOPK))
    route_weight = jnp.clip(0.1 + 0.5 * jax.random.uniform(seeds[3], (SERIES_ENTRIES, TOPK), jnp.float32) ** steps_of(seeds[3], (SERIES_ENTRIES, TOPK), ((0, 8),), -0.2, 0.2), 0.1, 0.6)
    gate_weight = gaussian(seeds[4], (EXPERTS, D, EXP_HIDDEN), D ** -0.5, 0.125, ((0, 8), (2, 4)))
    up_weight = gaussian(seeds[5], (EXPERTS, D, EXP_HIDDEN), D ** -0.5, 0.125, ((0, 8), (2, 4)))
    down_weight = gaussian(seeds[6], (EXPERTS, EXP_HIDDEN, D), EXP_HIDDEN ** -0.5, 0.1875, ((0, 8), (1, 4)))
    heads_value = gaussian(seeds[7], (SERIES_ENTRIES, SSD_W), 1.0, 6.0, ((0, 8), (1, 4)))
    output_gate = gaussian(seeds[8], (SERIES_ENTRIES, SSD_W), 1.5, 8.0, ((0, 8), (1, 4)))
    mixer_saved = gaussian(seeds[9], (SERIES_ENTRIES, SSD_W), 1.0, 6.0, ((0, 8), (1, 4)))
    proj_weight = gaussian(seeds[10], (D, SSD_W), SSD_W ** -0.5, 0.125, ((1, 4),))
    state_write = gaussian(seeds[11], (SERIES_ENTRIES, GROUPS * STATE), 0.08, 0.5, ((0, 8), (1, 4)))
    state_read = gaussian(seeds[12], (SERIES_ENTRIES, GROUPS * STATE), 0.08, 0.5, ((0, 8), (1, 4)))
    decay_rate = draw_decay_rate(jax.random.fold_in(seeds[14], 71), 0)
    return dict(layer_input=layer_input, cotangent=cotangent, routes=routes, route_weight=route_weight, gate_weight=gate_weight, up_weight=up_weight, down_weight=down_weight, heads_value=heads_value, output_gate=output_gate, mixer_saved=mixer_saved, proj_weight=proj_weight, state_write=state_write, state_read=state_read, decay_rate=decay_rate)


maximal_value = lax.Precision.HIGHEST


def silu_parts(value):
    sigma = jax.nn.sigmoid(value)
    return value * sigma, sigma * (1.0 + value * (1.0 - sigma))


def slot_index(flat_routes):
    onehot = (flat_routes[:, None] == jnp.arange(EXPERTS, dtype=jnp.int32)[None, :]).astype(jnp.int32)
    before = jnp.cumsum(onehot, axis=0, dtype=jnp.int32) - onehot
    ranks = jnp.sum(before * onehot, axis=1, dtype=jnp.int32)
    return (flat_routes * CAP + ranks).astype(jnp.int32)


def block_sums(block):
    value_vectors, step_deltas, write_vectors, read_vectors, rates = block
    repeat = BLENDER_CHANNEL // GROUPS
    cumul = jnp.cumsum(rates, axis=0)
    total = cumul[-1]
    to_end = jnp.exp(cumul - total)
    to_start = jnp.exp(-cumul)
    write_heads = jnp.repeat(write_vectors, repeat, axis=1)
    read_heads = jnp.repeat(read_vectors, repeat, axis=1)
    write_end = jnp.einsum('shn,shp->hnp', write_heads * to_end[:, :, None], value_vectors, precision=maximal_value)
    read_end = jnp.einsum('shn,shp->hnp', read_heads * to_end[:, :, None], step_deltas, precision=maximal_value)
    write_start = jnp.einsum('shn,shp->hnp', write_heads * to_start[:, :, None], value_vectors, precision=maximal_value)
    read_start = jnp.einsum('shn,shp->hnp', read_heads * to_start[:, :, None], step_deltas, precision=maximal_value)
    return total, write_end, read_end, write_start, read_start


def block_grads(item):
    value_vectors, step_deltas, write_vectors, read_vectors, rates, write_low, read_low, write_high, read_high = item
    repeat = BLENDER_CHANNEL // GROUPS
    length = value_vectors.shape[0]
    cumul = jnp.cumsum(rates, axis=0)
    to_end = jnp.exp(cumul - cumul[-1])
    to_start = jnp.exp(-cumul)
    write_heads = jnp.repeat(write_vectors, repeat, axis=1)
    read_heads = jnp.repeat(read_vectors, repeat, axis=1)
    mixing_kernel = jnp.exp(-jnp.abs(cumul.T[:, :, None] - cumul.T[:, None, :]))
    common_part = jnp.repeat(jnp.einsum('tgn,sgn->gts', read_vectors, write_vectors, precision=maximal_value), repeat, axis=0)
    match_scores = jnp.einsum('thp,shp->hts', step_deltas, value_vectors, precision=maximal_value)
    weighted_values = mixing_kernel * match_scores
    value_g = jnp.einsum('hts,thp->shp', mixing_kernel * common_part, step_deltas, precision=maximal_value)
    write_g = jnp.einsum('hts,thn->shn', weighted_values, read_heads, precision=maximal_value)
    read_g = jnp.einsum('hts,shn->thn', weighted_values, write_heads, precision=maximal_value)
    value_g = value_g + jnp.einsum('hnp,thn->thp', read_low, write_heads, precision=maximal_value) * to_start[:, :, None]
    value_g = value_g + jnp.einsum('hnp,thn->thp', read_high, write_heads, precision=maximal_value) * to_end[:, :, None]
    write_g = write_g + jnp.einsum('hnp,thp->thn', read_low, value_vectors * to_start[:, :, None], precision=maximal_value)
    write_g = write_g + jnp.einsum('hnp,thp->thn', read_high, value_vectors * to_end[:, :, None], precision=maximal_value)
    read_g = read_g + jnp.einsum('hnp,thp->thn', write_low, step_deltas * to_start[:, :, None], precision=maximal_value)
    read_g = read_g + jnp.einsum('hnp,thp->thn', write_high, step_deltas * to_end[:, :, None], precision=maximal_value)
    write_g = write_g.reshape(length, GROUPS, repeat, STATE).sum(axis=2)
    read_g = read_g.reshape(length, GROUPS, repeat, STATE).sum(axis=2)
    return value_g, write_g, read_g


def reference(layer_input, cotangent, routes, route_weight, gate_weight, up_weight, down_weight,
              heads_value, output_gate, mixer_saved, proj_weight, state_write, state_read, decay_rate):
    flat = routes.reshape(N_SP, TOK_DEV * TOPK)
    slots = jax.vmap(slot_index)(flat)
    owners = jnp.arange(TOK_DEV * TOPK, dtype=jnp.int32) // TOPK
    offsets = (jnp.arange(N_SP, dtype=jnp.int32) * TOK_DEV)[:, None]

    def slot_tokens(slot_row, offset_row):
        return jnp.full((EXPERTS * CAP,), SERIES_ENTRIES, jnp.int32).at[slot_row].set(owners + offset_row)

    def slot_weights(slot_row, weight_row):
        return jnp.zeros((EXPERTS * CAP,), jnp.float32).at[slot_row].set(weight_row)

    token_table = jax.vmap(slot_tokens)(slots, offsets)
    weight_table = jax.vmap(slot_weights)(slots, route_weight.reshape(N_SP, TOK_DEV * TOPK))
    token_table = token_table.reshape(N_SP, EXPERTS, CAP).transpose(1, 0, 2).reshape(EXPERTS, N_SP * CAP)
    weight_table = weight_table.reshape(N_SP, EXPERTS, CAP).transpose(1, 0, 2).reshape(EXPERTS, N_SP * CAP)
    inputs_pad = jnp.concatenate([layer_input, jnp.zeros((1, D), layer_input.dtype)], axis=0)
    cotangent_pad = jnp.concatenate([cotangent, jnp.zeros((1, D), cotangent.dtype)], axis=0)
    width = EXP_HIDDEN // N_TP

    def expert_step(item):
        rows, weights, gate_one, up_one, down_one = item
        inputs = inputs_pad[rows]
        sent = (cotangent_pad[rows].astype(jnp.float32) * weights[:, None]).astype(jnp.bfloat16)
        pre_gate = jnp.dot(inputs, gate_one, preferred_element_type=jnp.float32)
        pre_up = jnp.dot(inputs, up_one, preferred_element_type=jnp.float32)
        active, slope = silu_parts(pre_gate)
        hidden = (active * pre_up).astype(jnp.bfloat16)
        hidden_grad = jnp.dot(sent, down_one.T, preferred_element_type=jnp.float32)
        gate_delta = (hidden_grad * pre_up * slope).astype(jnp.bfloat16)
        up_delta = (hidden_grad * active).astype(jnp.bfloat16)
        down_g = jnp.dot(hidden.T, sent, preferred_element_type=jnp.float32).astype(jnp.bfloat16)
        gate_g = jnp.dot(inputs.T, gate_delta, preferred_element_type=jnp.float32).astype(jnp.bfloat16)
        up_g = jnp.dot(inputs.T, up_delta, preferred_element_type=jnp.float32).astype(jnp.bfloat16)
        parts = jnp.einsum('rjk,djk->jrd', gate_delta.reshape(-1, N_TP, width).astype(jnp.float32),
                           gate_one.reshape(D, N_TP, width).astype(jnp.float32))
        parts = parts + jnp.einsum('rjk,djk->jrd', up_delta.reshape(-1, N_TP, width).astype(jnp.float32),
                                   up_one.reshape(D, N_TP, width).astype(jnp.float32))
        rounded = lax.optimization_barrier(parts.astype(jnp.bfloat16)).astype(jnp.float32)
        returned = jnp.sum(rounded, axis=0).astype(jnp.bfloat16)
        return gate_g, up_g, down_g, returned

    gate_grad, up_grad, down_grad, returned = lax.map(
        expert_step, (token_table, weight_table, gate_weight, up_weight, down_weight))
    expert_of = slots // CAP
    rank_of = slots % CAP
    sources = jnp.arange(N_SP, dtype=jnp.int32)[:, None]
    position = (expert_of * (N_SP * CAP) + sources * CAP + rank_of).astype(jnp.int32).reshape(-1)
    moe_grad = returned.reshape(-1, D)[position].astype(jnp.float32).reshape(SERIES_ENTRIES, TOPK, D).sum(axis=1)
    layer_grad = (cotangent.astype(jnp.float32) + moe_grad).astype(jnp.bfloat16)

    out_delta = jnp.dot(layer_grad, proj_weight, preferred_element_type=jnp.float32).astype(jnp.bfloat16)
    active_gate, slope_gate = silu_parts(output_gate.astype(jnp.float32))
    saved = mixer_saved.astype(jnp.float32)
    gated = (saved * active_gate).astype(jnp.bfloat16)
    proj_grad = jnp.dot(layer_grad.T, gated, preferred_element_type=jnp.float32)
    outgate_grad = (out_delta.astype(jnp.float32) * saved * slope_gate).astype(jnp.bfloat16)
    mixer_delta = out_delta.astype(jnp.float32) * active_gate

    blk = math.gcd(TOK_DEV, 256)
    count = SERIES_ENTRIES // blk
    value_vectors = heads_value.astype(jnp.float32).reshape(count, blk, BLENDER_CHANNEL, HEAD_DIM)
    step_deltas = mixer_delta.reshape(count, blk, BLENDER_CHANNEL, HEAD_DIM)
    write_vectors = state_write.astype(jnp.float32).reshape(count, blk, GROUPS, STATE)
    read_vectors = state_read.astype(jnp.float32).reshape(count, blk, GROUPS, STATE)
    rates = decay_rate.astype(jnp.float32).reshape(count, blk, BLENDER_CHANNEL)
    totals, write_end, read_end, write_start, read_start = lax.map(block_sums, (value_vectors, step_deltas, write_vectors, read_vectors, rates))
    zero_state = jnp.zeros((BLENDER_CHANNEL, STATE, HEAD_DIM), jnp.float32)

    def carry_on(state, item):
        total, write_part, read_part = item
        fade = jnp.exp(-total)[:, None, None]
        return (fade * state[0] + write_part, fade * state[1] + read_part), state

    _, (write_low, read_low) = lax.scan(carry_on, (zero_state, zero_state), (totals, write_end, read_end))
    _, (write_high, read_high) = lax.scan(carry_on, (zero_state, zero_state), (totals, write_start, read_start), reverse=True)
    value_g, write_g, read_g = lax.map(block_grads, (value_vectors, step_deltas, write_vectors, read_vectors, rates,
                                                     write_low, read_low, write_high, read_high))
    return (gate_grad, up_grad, down_grad, proj_grad,
            value_g.reshape(SERIES_ENTRIES, SSD_W).astype(jnp.bfloat16),
            write_g.reshape(SERIES_ENTRIES, GROUPS * STATE).astype(jnp.bfloat16),
            read_g.reshape(SERIES_ENTRIES, GROUPS * STATE).astype(jnp.bfloat16),
            outgate_grad)
```

```python
import functools

import jax
import jax.numpy as jnp
from jax import lax
from jax.experimental import pallas as pl
from jax.experimental.pallas import tpu as pltpu
from jax.sharding import PartitionSpec as P

HEAD_DIM = 64
STATE = 128
MESH = pl.DeviceIdType.MESH
LAST = (((1,), (1,)), ((), ()))
FIRST = (((0,), (0,)), ((), ()))
F32 = jnp.float32
BF16 = jnp.bfloat16
VMEM = pltpu.VMEM
DMA = pltpu.SemaphoreType.DMA


def silu_parts(value):
    sigma = jax.nn.sigmoid(value)
    return (value * sigma, sigma * (1.0 + value * (1.0 - sigma)))


class Place:
    def __init__(self, n, t):
        self.n, self.t = n, t
        self.sp = lax.axis_index("sp")
        self.tp = lax.axis_index("tp")
        self.across = lax.rem(self.tp + t // 2, t)
        self.beside = self.tp + 1 - 2 * lax.rem(self.tp, 2)
        self.cross = lax.rem(self.beside + t // 2, t)

    def to(self, src, dst, send, recv, sp=None, tp=None):
        return pltpu.make_async_remote_copy(
            src_ref=src,
            dst_ref=dst,
            send_sem=send,
            recv_sem=recv,
            device_id=(self.sp if sp is None else sp, self.tp if tp is None else tp),
            device_id_type=MESH,
        )

    def greet(self, sp_too=True):
        barrier = pltpu.get_barrier_semaphore()
        for tp in (self.across, self.beside):
            pl.semaphore_signal(barrier, inc=1, device_id=(self.sp, tp), device_id_type=MESH)
        count = 2
        if sp_too:
            for o in range(1, self.n):
                pl.semaphore_signal(
                    barrier,
                    inc=1,
                    device_id=(lax.rem(self.sp + o, self.n), self.tp),
                    device_id_type=MESH,
                )
            count += self.n - 1
        pl.semaphore_wait(barrier, count)


def loop(lo, hi, body):
    def step(i, carry):
        body(i)
        return carry

    lax.fori_loop(lo, hi, step, 0)


def dispatch_kernel(
    n, t, x_ref, c_ref, a_ref, xo, co, ao, s_a2a, r_a2a, s_sh, r_sh, s_d, r_d, own_sem
):
    at = Place(n, t)
    d = x_ref.shape[2]
    col = lambda tp: pl.ds(pl.multiple_of(tp * d, d), d)
    sides = ((x_ref, xo), (c_ref, co))
    at.greet()

    def spread(k, o):
        src, dst = sides[k]
        peer = lax.rem(at.sp + o, n)
        return at.to(
            src.at[peer], dst.at[at.sp, :, col(at.tp)], s_a2a.at[k, o], r_a2a.at[k, o], sp=peer
        )

    def decay(o):
        peer = lax.rem(at.sp + o, n)
        return at.to(a_ref, ao.at[at.sp], s_d.at[o], r_d.at[o], sp=peer)

    def share(k, o, j):
        here = sides[k][1].at[lax.rem(at.sp + n - o, n), :, col(at.across if j == 2 else at.tp)]
        return at.to(
            here, here, s_sh.at[k, j, o], r_sh.at[k, j, o], tp=at.across if j == 0 else at.beside
        )

    owns = [
        pltpu.make_async_copy(
            src.at[at.sp], dst.at[at.sp, :, col(at.tp)], own_sem.at[k]
        )
        for k, (src, dst) in enumerate(sides)
    ]
    owns.append(pltpu.make_async_copy(a_ref, ao.at[at.sp], own_sem.at[2]))
    for own in owns:
        own.start()
    for k in (0, 1):
        loop(1, n, lambda o: spread(k, o).start())
    loop(1, n, lambda o: decay(o).start())
    for k in (0, 1):
        owns[k].wait()
        share(k, 0, 0).start()
        share(k, 0, 1).start()
    owns[2].wait()
    for k in (0, 1):

        def arrive(o):
            spread(k, o).wait_recv()
            share(k, o, 0).start()
            share(k, o, 1).start()
            share(k, o - 1, 0).wait_recv()
            share(k, o - 1, 2).start()

        loop(1, n, arrive)
        share(k, n - 1, 0).wait_recv()
        share(k, n - 1, 2).start()

    def finish(o):
        for k in (0, 1):
            share(k, o, 1).wait_recv()
            share(k, o, 2).wait_recv()
            for j in (0, 1, 2):
                share(k, o, j).wait_send()

    loop(0, n, finish)

    def finish_spread(o):
        for k in (0, 1):
            spread(k, o).wait_send()
        decay(o).wait()

    loop(1, n, finish_spread)


def combine_kernel(n, t, p_ref, out, pair, summed, other, final, s_p, r_p, s_y, r_y, s_a, r_a, own):
    at = Place(n, t)
    d = out.shape[2]
    col = lambda tp: pl.ds(pl.multiple_of(tp * d, d), d)
    at.greet()
    halves = [
        at.to(p_ref.at[:, :, col(c)], pair.at[k], s_p.at[k], r_p.at[k], tp=at.beside)
        for k, c in enumerate((at.cross, at.beside))
    ]
    for half in halves:
        half.start()

    def over(o):
        b = lax.rem(at.sp + o, n)
        return at.to(summed.at[b], other.at[b], s_y.at[o], r_y.at[o], tp=at.across)

    def back(o):
        b = lax.rem(at.sp + o, n)
        return at.to(final.at[b], out.at[at.sp], s_a.at[o], r_a.at[o], sp=b)

    halves[0].wait_recv()

    def add_pair(o):
        b = lax.rem(at.sp + o, n)
        summed[b] = (
            p_ref[b, :, col(at.across)].astype(F32) + pair[0, b].astype(F32)
        ).astype(BF16)
        over(o).start()

    def turn(i):
        o = i + 1
        add_pair(lax.rem(o, n))

    loop(0, n, turn)
    halves[1].wait_recv()

    def total(o):
        b = lax.rem(at.sp + o, n)
        over(o).wait_recv()
        final[b] = (
            p_ref[b, :, col(at.tp)].astype(F32) + pair[1, b].astype(F32) + other[b].astype(F32)
        ).astype(BF16)

    def total_and_send(o):
        total(o)
        back(o).start()

    loop(1, n, total_and_send)
    total(0)
    mine = pltpu.make_async_copy(final.at[at.sp], out.at[at.sp], own.at[0])
    mine.start()
    mine.wait()
    for half in halves:
        half.wait_send()
    loop(0, n, lambda o: over(o).wait_send())
    loop(1, n, lambda o: back(o).wait())


def rows_kernel(n, t, g_ref, out, s_sh, r_sh, own):
    at = Place(n, t)
    d = g_ref.shape[1]
    col = lambda tp: pl.ds(pl.multiple_of(tp * d, d), d)
    at.greet(sp_too=False)
    mine = pltpu.make_async_copy(g_ref, out.at[:, col(at.tp)], own.at[0])
    mine.start()
    first = at.to(g_ref, out.at[:, col(at.tp)], s_sh.at[0], r_sh.at[0], tp=at.across)
    side = at.to(g_ref, out.at[:, col(at.tp)], s_sh.at[1], r_sh.at[1], tp=at.beside)
    first.start()
    side.start()
    here = out.at[:, col(at.across)]
    onward = at.to(here, here, s_sh.at[2], r_sh.at[2], tp=at.beside)
    first.wait_recv()
    onward.start()
    mine.wait()
    side.wait()
    first.wait_send()
    onward.wait()


def late_kernel(
    n, t, d_ref, g_ref, dall, gall, s_g, r_g, s_sh, r_sh, s_x, r_x, s_l, r_l, own
):
    at = Place(n, t)
    q = g_ref.shape[1] // t
    row = lambda tp: pl.ds(pl.multiple_of(tp * q, q), q)
    length = n // 2
    z = at.sp // 2
    bit = lax.rem(at.sp, 2)
    at.greet()
    mine = pltpu.make_async_copy(d_ref, dall.at[at.sp], own.at[0])
    mine.start()
    keep = pltpu.make_async_copy(g_ref.at[at.sp], gall.at[at.sp], own.at[1])
    keep.start()
    twin = z * 2 + 1 - bit
    pair = at.to(d_ref, dall.at[at.sp], s_x.at[0], r_x.at[0], sp=twin)
    pair.start()

    def spread(o):
        peer = lax.rem(at.sp + o, n)
        return at.to(
            g_ref.at[peer, row(at.tp), :],
            gall.at[at.sp, row(at.tp), :],
            s_g.at[o],
            r_g.at[o],
            sp=peer,
        )

    def share(o, j):
        here = gall.at[lax.rem(at.sp + n - o, n), row(at.across if j == 2 else at.tp), :]
        return at.to(
            here, here, s_sh.at[j, o], r_sh.at[j, o], tp=at.across if j == 0 else at.beside
        )

    def hop(up, k, same):
        source = z - k if up else z + k
        block = source * 2 + (bit if same else 1 - bit)
        direction = 0 if up else 1
        which = 0 if same else 1
        peer = z + 1 if up else z - 1
        return at.to(
            dall.at[block],
            dall.at[block],
            s_l.at[direction, which, k],
            r_l.at[direction, which, k],
            sp=peer * 2 + bit,
        )

    def came(up, k, same):
        source = z - k if up else z + k
        block = source * 2 + (bit if same else 1 - bit)
        return at.to(
            dall.at[block],
            dall.at[block],
            s_l.at[0 if up else 1, 0 if same else 1, k],
            r_l.at[0 if up else 1, 0 if same else 1, k - 1],
            sp=twin,
        )

    loop(1, n, lambda o: spread(o).start())
    mine.wait()
    for same in (True, False):
        if not same:
            pair.wait_recv()

        @pl.when(z < length - 1)
        def _():
            hop(True, 0, same).start()

        @pl.when(z > 0)
        def _():
            hop(False, 0, same).start()

    def arrive(o):
        spread(o).wait_recv()
        share(o, 0).start()
        share(o, 1).start()

    loop(1, n, arrive)
    keep.wait()
    for k in range(1, length):
        for same in (True, False):

            @pl.when(z - k >= 0)
            def _():
                came(True, k, same).wait_recv()

                @pl.when(z < length - 1)
                def _():
                    hop(True, k, same).start()

            @pl.when(z + k < length)
            def _():
                came(False, k, same).wait_recv()

                @pl.when(z > 0)
                def _():
                    hop(False, k, same).start()

    def onward(o):
        share(o, 0).wait_recv()
        share(o, 2).start()

    loop(1, n, onward)

    def finish(o):
        share(o, 1).wait_recv()
        share(o, 2).wait_recv()
        for j in (0, 1, 2):
            share(o, j).wait_send()
        spread(o).wait_send()

    loop(1, n, finish)
    for k in range(length):
        for same in (True, False):

            @pl.when(jnp.logical_and(z - k >= 0, z < length - 1))
            def _():
                hop(True, k, same).wait_send()

            @pl.when(jnp.logical_and(z + k < length, z > 0))
            def _():
                hop(False, k, same).wait_send()

    pair.wait_send()


def mixer_kernel(chunk, dall, vall, rall, wall, arow, acol, dl, vl, rl, wl, vg, wg, rg):
    heads = acol.shape[1]
    per = heads * STATE // wl.shape[1]
    total = dall.shape[0]
    vg_sum = [jnp.zeros((dl.shape[0], HEAD_DIM), F32) for _ in range(heads)]
    wg_sum = [jnp.zeros((dl.shape[0], STATE), F32) for _ in range(heads // per)]
    rg_sum = [jnp.zeros((dl.shape[0], STATE), F32) for _ in range(heads // per)]

    def dot_last(a, b):
        return lax.dot_general(a, b, LAST, preferred_element_type=F32)

    def step(i, carry):
        vg_sum, wg_sum, rg_sum = carry
        vg_sum, wg_sum, rg_sum = list(vg_sum), list(wg_sum), list(rg_sum)
        rows = pl.ds(pl.multiple_of(i * chunk, chunk), chunk)
        for g in range(heads // per):
            wide = slice(g * STATE, (g + 1) * STATE)
            read, write = rall[rows, wide], wall[rows, wide]
            common = dot_last(wl[:, wide], read)
            q1 = jnp.zeros((dl.shape[0], chunk), F32)
            q2 = jnp.zeros((dl.shape[0], chunk), F32)
            for h in range(g * per, (g + 1) * per):
                cols = slice(h * HEAD_DIM, (h + 1) * HEAD_DIM)
                delta, value = dall[rows, cols], vall[rows, cols]
                fade = jnp.exp(-jnp.abs(acol[:, h : h + 1] - arow[h : h + 1, rows]))
                vg_sum[h] += jnp.dot(
                    (fade * common).astype(BF16), delta, preferred_element_type=F32
                )
                q1 += fade * dot_last(vl[:, cols], delta)
                q2 += fade * dot_last(dl[:, cols], value)
            wg_sum[g] += jnp.dot(q1.astype(BF16), read, preferred_element_type=F32)
            rg_sum[g] += jnp.dot(q2.astype(BF16), write, preferred_element_type=F32)
        return tuple(vg_sum), tuple(wg_sum), tuple(rg_sum)

    vg_sum, wg_sum, rg_sum = lax.fori_loop(
        0, total // chunk, step, (tuple(vg_sum), tuple(wg_sum), tuple(rg_sum))
    )
    for h in range(heads):
        vg[:, h * HEAD_DIM : (h + 1) * HEAD_DIM] = vg_sum[h].astype(BF16)
    for g in range(heads // per):
        wg[:, g * STATE : (g + 1) * STATE] = wg_sum[g].astype(BF16)
        rg[:, g * STATE : (g + 1) * STATE] = rg_sum[g].astype(BF16)


def call(kernel, ident, ins, outs, scratch, operands, name):
    vm = pl.BlockSpec(memory_space=pltpu.VMEM)
    return pl.pallas_call(
        kernel,
        out_shape=outs,
        in_specs=[vm] * ins,
        out_specs=jax.tree.map(lambda _: vm, outs),
        scratch_shapes=scratch,
        compiler_params=pltpu.CompilerParams(
            collective_id=ident,
            has_side_effects=ident is not None,
            vmem_limit_bytes=56 * 1024 * 1024,
        ),
        cost_estimate=pl.CostEstimate(
            flops=4_000_000_000, bytes_accessed=8_000_000, transcendentals=0
        ),
        name=name,
    )(*operands)


def on_device(
    layer_input,
    cotangent,
    routes,
    route_weight,
    gate_weight,
    up_weight,
    down_weight,
    heads_value,
    output_gate,
    mixer_saved,
    proj_weight,
    state_write,
    state_read,
    decay_rate,
):
    n = lax.axis_size("sp")
    t = lax.axis_size("tp")
    me = lax.axis_index("sp")
    tokens, d = layer_input.shape
    top = routes.shape[1]
    capacity = max(2, 3 * tokens * top // (2 * n))
    slots_all = n * capacity
    sds = jax.ShapeDtypeStruct

    active_gate, slope_gate = silu_parts(output_gate.astype(F32))
    saved = mixer_saved.astype(F32)
    gated = (saved * active_gate).astype(BF16)
    packed = jnp.concatenate([heads_value, gated, state_write, state_read], axis=1)
    everything = lax.all_gather(packed, "sp", axis=0, tiled=True)

    flat = routes.reshape(-1)
    count = flat.shape[0]
    onehot = (flat[:, None] == jnp.arange(n, dtype=jnp.int32)[None, :]).astype(BF16)
    lower = (
        jnp.arange(count, dtype=jnp.int32)[:, None] > jnp.arange(count, dtype=jnp.int32)[None, :]
    ).astype(BF16)
    before = jnp.dot(lower, onehot, preferred_element_type=F32)
    ranks = jnp.sum(before * onehot.astype(F32), axis=1).astype(jnp.int32)
    slots = (flat * capacity + ranks).reshape(tokens, top)
    slot_ids = jnp.arange(slots_all, dtype=jnp.int32)
    hits = [(slots[:, k][None, :] == slot_ids[:, None]) for k in range(top)]
    pick = functools.reduce(jnp.logical_or, hits).astype(BF16)
    slot_weight = sum(
        jnp.sum(jnp.where(hits[k], route_weight[:, k][None, :], 0.0), axis=1) for k in range(top)
    )
    send_input = (
        jnp.dot(pick, layer_input, preferred_element_type=F32)
        .astype(BF16)
        .reshape(n, capacity, d)
    )
    send_cotangent = (
        (jnp.dot(pick, cotangent, preferred_element_type=F32) * slot_weight[:, None])
        .astype(BF16)
        .reshape(n, capacity, d)
    )
    decay_sum = jnp.cumsum(decay_rate, axis=0).T
    heads = decay_sum.shape[0]

    expert_input, expert_cotangent, decays = call(
        functools.partial(dispatch_kernel, n, t),
        1,
        3,
        (
            sds((n, capacity, t * d), BF16),
            sds((n, capacity, t * d), BF16),
            sds((n, heads, tokens), F32),
        ),
        [
            DMA((2, n)),
            DMA((2, n)),
            DMA((2, 3, n)),
            DMA((2, 3, n)),
            DMA((n,)),
            DMA((n,)),
            DMA((3,)),
        ],
        (send_input, send_cotangent, decay_sum),
        "dispatch",
    )
    expert_input = expert_input.reshape(slots_all, t * d)
    expert_cotangent = expert_cotangent.reshape(slots_all, t * d)
    gate_local = gate_weight[0]
    up_local = up_weight[0]
    down_local = down_weight[0]
    pre_gate = jnp.dot(expert_input, gate_local, preferred_element_type=F32)
    pre_up = jnp.dot(expert_input, up_local, preferred_element_type=F32)
    active, slope = silu_parts(pre_gate)
    hidden = (active * pre_up).astype(BF16)
    hidden_grad = lax.dot_general(expert_cotangent, down_local, LAST, preferred_element_type=F32)
    gate_delta = (hidden_grad * pre_up * slope).astype(BF16)
    up_delta = (hidden_grad * active).astype(BF16)
    partial_grad = lax.dot_general(gate_delta, gate_local, LAST, preferred_element_type=F32)
    partial_grad = partial_grad + lax.dot_general(
        up_delta, up_local, LAST, preferred_element_type=F32
    )
    partial_grad = partial_grad.astype(BF16).reshape(n, capacity, t * d)
    block = (n, capacity, d)
    arrived = call(
        functools.partial(combine_kernel, n, t),
        2,
        1,
        sds(block, BF16),
        [
            VMEM((2,) + block, BF16),
            VMEM(block, BF16),
            VMEM(block, BF16),
            VMEM(block, BF16),
            DMA((2,)),
            DMA((2,)),
            DMA((n,)),
            DMA((n,)),
            DMA((n,)),
            DMA((n,)),
            DMA((1,)),
        ],
        (partial_grad,),
        "combine",
    ).reshape(slots_all, d)
    moe_grad = lax.dot_general(pick, arrived, FIRST, preferred_element_type=F32)
    layer_grad = (cotangent.astype(F32) + moe_grad).astype(BF16)
    full_grad = call(
        functools.partial(rows_kernel, n, t),
        3,
        1,
        sds((tokens, t * d), BF16),
        [DMA((3,)), DMA((3,)), DMA((1,))],
        (layer_grad,),
        "rows",
    )
    out_delta = jnp.dot(full_grad, proj_weight, preferred_element_type=F32).astype(BF16)
    outgate_grad = (out_delta.astype(F32) * saved * slope_gate).astype(BF16)
    mixer_delta = (out_delta.astype(F32) * active_gate).astype(BF16)
    width = t * d // n
    by_owner = full_grad.reshape(tokens, n, width).transpose(1, 0, 2)
    length = max(1, n // 2)
    all_delta, all_grad = call(
        functools.partial(late_kernel, n, t),
        4,
        2,
        (sds((n, tokens, d), BF16), sds((n, tokens, width), BF16)),
        [
            DMA((n,)),
            DMA((n,)),
            DMA((3, n)),
            DMA((3, n)),
            DMA((1,)),
            DMA((1,)),
            DMA((2, 2, length)),
            DMA((2, 2, length)),
            DMA((2,)),
        ],
        (mixer_delta, by_owner),
        "late",
    )

    down_grad = lax.dot_general(hidden, expert_cotangent, FIRST, preferred_element_type=F32)
    gate_grad = lax.dot_general(expert_input, gate_delta, FIRST, preferred_element_type=F32)
    up_grad = lax.dot_general(expert_input, up_delta, FIRST, preferred_element_type=F32)

    all_value = everything[:, :d]
    all_gated = everything[:, d : 2 * d]
    state_w = state_write.shape[1]
    all_write = everything[:, 2 * d : 2 * d + state_w]
    all_read = everything[:, 2 * d + state_w :]
    proj_grad = lax.dot_general(
        all_grad.reshape(n * tokens, width), all_gated, FIRST, preferred_element_type=F32
    )
    totals = decays[:, :, -1]
    start = jnp.cumsum(totals, axis=0) - totals
    decay_row = (decays + start[:, :, None]).transpose(1, 0, 2)
    decay_here = lax.dynamic_index_in_dim(decay_row, me, axis=1, keepdims=False).T
    chunk = min(4, n) * tokens
    value_grad, write_gradient, read_gradient = call(
        functools.partial(mixer_kernel, chunk),
        None,
        10,
        (sds((tokens, d), BF16), sds((tokens, state_w), BF16), sds((tokens, state_w), BF16)),
        [],
        (
            all_delta.reshape(n * tokens, d),
            all_value,
            all_read,
            all_write,
            decay_row.reshape(heads, n * tokens),
            decay_here,
            mixer_delta,
            heads_value,
            state_read,
            state_write,
        ),
        "mixer",
    )
    return (
        gate_grad.astype(BF16)[None],
        up_grad.astype(BF16)[None],
        down_grad.astype(BF16)[None],
        proj_grad,
        value_grad,
        write_gradient,
        read_gradient,
        outgate_grad,
    )


def solution(mesh):
    split = P("sp", "tp")
    in_specs = (
        split,
        split,
        P("sp", None),
        P("sp", None),
        P("sp", None, "tp"),
        P("sp", None, "tp"),
        P("sp", "tp", None),
        split,
        split,
        split,
        P(None, "tp"),
        split,
        split,
        split,
    )
    out_specs = (
        P("sp", None, "tp"),
        P("sp", None, "tp"),
        P("sp", "tp", None),
        split,
        split,
        split,
        split,
        split,
    )
    return jax.shard_map(
        on_device, mesh=mesh, in_specs=in_specs, out_specs=out_specs, check_vma=False
    )
```

```python
import functools

import jax
import jax.numpy as jnp
from jax import lax
from jax.experimental import pallas as pl
from jax.experimental.pallas import tpu as pltpu
from jax.sharding import PartitionSpec as P

HEAD_DIM = 64
STATE = 128
MESH = pl.DeviceIdType.MESH
LAST = (((1,), (1,)), ((), ()))
FIRST = (((0,), (0,)), ((), ()))
F32 = jnp.float32
BF16 = jnp.bfloat16
VMEM = pltpu.VMEM
DMA = pltpu.SemaphoreType.DMA


def silu_parts(value):
    sigma = jax.nn.sigmoid(value)
    return (value * sigma, sigma * (1.0 + value * (1.0 - sigma)))


class Place:
    def __init__(self, n, t):
        self.n, self.t = n, t
        self.sp = lax.axis_index("sp")
        self.tp = lax.axis_index("tp")
        self.across = lax.rem(self.tp + t // 2, t)
        self.beside = self.tp + 1 - 2 * lax.rem(self.tp, 2)
        self.cross = lax.rem(self.beside + t // 2, t)

    def to(self, src, dst, send, recv, sp=None, tp=None):
        return pltpu.make_async_remote_copy(
            src_ref=src,
            dst_ref=dst,
            send_sem=send,
            recv_sem=recv,
            device_id=(self.sp if sp is None else sp, self.tp if tp is None else tp),
            device_id_type=MESH,
        )

    def greet(self, sp_too=True):
        barrier = pltpu.get_barrier_semaphore()
        for tp in (self.across, self.beside):
            pl.semaphore_signal(barrier, inc=1, device_id=(self.sp, tp), device_id_type=MESH)
        count = 2
        if sp_too:
            for o in range(1, self.n):
                pl.semaphore_signal(
                    barrier,
                    inc=1,
                    device_id=(lax.rem(self.sp + o, self.n), self.tp),
                    device_id_type=MESH,
                )
            count += self.n - 1
        pl.semaphore_wait(barrier, count)


def loop(lo, hi, body):
    def step(i, carry):
        body(i)
        return carry

    lax.fori_loop(lo, hi, step, 0)


def dispatch_kernel(
    n, t, x_ref, c_ref, a_ref, xo, co, ao, s_a2a, r_a2a, s_sh, r_sh, s_d, r_d, own_sem
):
    at = Place(n, t)
    d = x_ref.shape[2]
    col = lambda tp: pl.ds(pl.multiple_of(tp * d, d), d)
    sides = ((x_ref, xo), (c_ref, co))
    at.greet()

    def spread(k, o):
        src, dst = sides[k]
        peer = lax.rem(at.sp + o, n)
        return at.to(
            src.at[peer], dst.at[at.sp, :, col(at.tp)], s_a2a.at[k, o], r_a2a.at[k, o], sp=peer
        )

    def decay(o):
        peer = lax.rem(at.sp + o, n)
        return at.to(a_ref, ao.at[at.sp], s_d.at[o], r_d.at[o], sp=peer)

    def share(k, o, j):
        here = sides[k][1].at[lax.rem(at.sp + n - o, n), :, col(at.across if j == 2 else at.tp)]
        return at.to(
            here, here, s_sh.at[k, j, o], r_sh.at[k, j, o], tp=at.across if j == 0 else at.beside
        )

    owns = [
        pltpu.make_async_copy(
            src.at[at.sp], dst.at[at.sp, :, col(at.tp)], own_sem.at[k]
        )
        for k, (src, dst) in enumerate(sides)
    ]
    owns.append(pltpu.make_async_copy(a_ref, ao.at[at.sp], own_sem.at[2]))
    for own in owns:
        own.start()
    for k in (0, 1):
        loop(1, n, lambda o: spread(k, o).start())
    loop(1, n, lambda o: decay(o).start())
    for k in (0, 1):
        owns[k].wait()
        share(k, 0, 0).start()
        share(k, 0, 1).start()
    owns[2].wait()
    for k in (0, 1):

        def arrive(o):
            spread(k, o).wait_recv()
            share(k, o, 0).start()
            share(k, o, 1).start()
            share(k, o - 1, 0).wait_recv()
            share(k, o - 1, 2).start()

        loop(1, n, arrive)
        share(k, n - 1, 0).wait_recv()
        share(k, n - 1, 2).start()

    def finish(o):
        for k in (0, 1):
            share(k, o, 1).wait_recv()
            share(k, o, 2).wait_recv()
            for j in (0, 1, 2):
                share(k, o, j).wait_send()

    loop(0, n, finish)

    def finish_spread(o):
        for k in (0, 1):
            spread(k, o).wait_send()
        decay(o).wait()

    loop(1, n, finish_spread)


def combine_kernel(n, t, p_ref, out, pair, summed, other, final, s_p, r_p, s_y, r_y, s_a, r_a, own):
    at = Place(n, t)
    d = out.shape[2]
    col = lambda tp: pl.ds(pl.multiple_of(tp * d, d), d)
    at.greet()
    halves = [
        at.to(p_ref.at[:, :, col(c)], pair.at[k], s_p.at[k], r_p.at[k], tp=at.beside)
        for k, c in enumerate((at.cross, at.beside))
    ]
    for half in halves:
        half.start()

    def over(o):
        b = lax.rem(at.sp + o, n)
        return at.to(summed.at[b], other.at[b], s_y.at[o], r_y.at[o], tp=at.across)

    def back(o):
        b = lax.rem(at.sp + o, n)
        return at.to(final.at[b], out.at[at.sp], s_a.at[o], r_a.at[o], sp=b)

    halves[0].wait_recv()

    def add_pair(o):
        b = lax.rem(at.sp + o, n)
        summed[b] = (
            p_ref[b, :, col(at.across)].astype(F32) + pair[0, b].astype(F32)
        ).astype(BF16)
        over(o).start()

    def turn(i):
        o = i + 1
        add_pair(lax.rem(o, n))

    loop(0, n, turn)
    halves[1].wait_recv()

    def total(o):
        b = lax.rem(at.sp + o, n)
        over(o).wait_recv()
        final[b] = (
            p_ref[b, :, col(at.tp)].astype(F32) + pair[1, b].astype(F32) + other[b].astype(F32)
        ).astype(BF16)

    def total_and_send(o):
        total(o)
        back(o).start()

    loop(1, n, total_and_send)
    total(0)
    mine = pltpu.make_async_copy(final.at[at.sp], out.at[at.sp], own.at[0])
    mine.start()
    mine.wait()
    for half in halves:
        half.wait_send()
    loop(0, n, lambda o: over(o).wait_send())
    loop(1, n, lambda o: back(o).wait())


def rows_kernel(n, t, g_ref, out, s_sh, r_sh, own):
    at = Place(n, t)
    d = g_ref.shape[1]
    col = lambda tp: pl.ds(pl.multiple_of(tp * d, d), d)
    at.greet(sp_too=False)
    mine = pltpu.make_async_copy(g_ref, out.at[:, col(at.tp)], own.at[0])
    mine.start()
    first = at.to(g_ref, out.at[:, col(at.tp)], s_sh.at[0], r_sh.at[0], tp=at.across)
    side = at.to(g_ref, out.at[:, col(at.tp)], s_sh.at[1], r_sh.at[1], tp=at.beside)
    first.start()
    side.start()
    here = out.at[:, col(at.across)]
    onward = at.to(here, here, s_sh.at[2], r_sh.at[2], tp=at.beside)
    first.wait_recv()
    onward.start()
    mine.wait()
    side.wait()
    first.wait_send()
    onward.wait()


def late_kernel(n, t, *refs):
    wide = (1, 2)
    count = 5
    ins, g_ref, outs, gall = refs[:count], refs[count], refs[6 : 6 + count], refs[11]
    s_g, r_g, s_sh, r_sh, s_x, r_x, s_l, r_l, s_t, r_t, own = refs[12:]
    at = Place(n, t)
    q = g_ref.shape[1] // t
    row = lambda tp: pl.ds(pl.multiple_of(tp * q, q), q)
    length = n // 2
    z = at.sp // 2
    bit = lax.rem(at.sp, 2)
    twin = z * 2 + 1 - bit
    at.greet()
    keeps = [
        pltpu.make_async_copy(ins[a], outs[a].at[at.sp], own.at[a]) for a in range(count)
    ]
    keeps.append(pltpu.make_async_copy(g_ref.at[at.sp], gall.at[at.sp], own.at[count]))
    for keep in keeps:
        keep.start()
    pairs = [
        at.to(ins[a], outs[a].at[at.sp], s_x.at[a], r_x.at[a], sp=twin) for a in range(count)
    ]

    def spread(o):
        peer = lax.rem(at.sp + o, n)
        return at.to(
            g_ref.at[peer, row(at.tp), :],
            gall.at[at.sp, row(at.tp), :],
            s_g.at[o],
            r_g.at[o],
            sp=peer,
        )

    def share(o, j):
        here = gall.at[lax.rem(at.sp + n - o, n), row(at.across if j == 2 else at.tp), :]
        return at.to(
            here, here, s_sh.at[j, o], r_sh.at[j, o], tp=at.across if j == 0 else at.beside
        )

    def block_of(up, k, same):
        return (z - k if up else z + k) * 2 + (bit if same else 1 - bit)

    def hop(a, up, k, same):
        here = outs[a].at[block_of(up, k, same)]
        i, j = (0 if up else 1), (0 if same else 1)
        peer = z + 1 if up else z - 1
        return at.to(here, here, s_l.at[a, i, j, k], r_l.at[a, i, j, k], sp=peer * 2 + bit)

    def came(a, up, k, same):
        here = outs[a].at[block_of(up, k, same)]
        i, j = (0 if up else 1), (0 if same else 1)
        return at.to(here, here, s_l.at[a, i, j, k], r_l.at[a, i, j, k - 1], sp=twin)

    def side(a, up, k):
        here = outs[a].at[block_of(up, k, True)]
        i = 0 if up else 1
        return at.to(here, here, s_t.at[a, i, k], r_t.at[a, i, k], sp=twin)

    def sides_of(a):
        return (True,) if a in wide else (True, False)

    for a in range(count):
        if a not in wide:
            pairs[a].start()
    loop(1, n, lambda o: spread(o).start())
    order = wide + tuple(a for a in range(count) if a not in wide)

    def begin(a, same):
        @pl.when(z < length - 1)
        def _():
            hop(a, True, 0, same).start()

        @pl.when(z > 0)
        def _():
            hop(a, False, 0, same).start()

    for a in order:
        keeps[a].wait()
        begin(a, True)
    for a in order:
        if a in wide:
            pairs[a].start()
        else:
            pairs[a].wait_recv()
            begin(a, False)

    def arrive(o):
        spread(o).wait_recv()
        share(o, 0).start()
        share(o, 1).start()

    def advance(k):
        for a in order:
            for same in sides_of(a):

                @pl.when(z - k >= 0)
                def _():
                    came(a, True, k, same).wait_recv()

                    @pl.when(z < length - 1)
                    def _():
                        hop(a, True, k, same).start()

                    if a in wide:
                        side(a, True, k).start()

                @pl.when(z + k < length)
                def _():
                    came(a, False, k, same).wait_recv()

                    @pl.when(z > 0)
                    def _():
                        hop(a, False, k, same).start()

                    if a in wide:
                        side(a, False, k).start()

    loop(1, length, advance)
    keeps[count].wait()
    loop(1, n, arrive)

    def onward(o):
        share(o, 0).wait_recv()
        share(o, 2).start()

    loop(1, n, onward)

    def finish(o):
        share(o, 1).wait_recv()
        share(o, 2).wait_recv()
        for j in (0, 1, 2):
            share(o, j).wait_send()
        spread(o).wait_send()

    loop(1, n, finish)

    def drain(k):
        for a in order:
            for same in sides_of(a):

                @pl.when(jnp.logical_and(z - k >= 0, z < length - 1))
                def _():
                    hop(a, True, k, same).wait_send()

                @pl.when(jnp.logical_and(z + k < length, z > 0))
                def _():
                    hop(a, False, k, same).wait_send()

    loop(0, length, drain)

    def settle(k):
        for a in wide:

            @pl.when(z - k >= 0)
            def _():
                side(a, True, k).wait()

            @pl.when(z + k < length)
            def _():
                side(a, False, k).wait()

    loop(1, length, settle)
    for a in range(count):
        if a in wide:
            pairs[a].wait_recv()
        pairs[a].wait_send()


def mixer_kernel(chunk, dall, vall, rall, wall, arow, acol, dl, vl, rl, wl, vg, wg, rg):
    heads = acol.shape[1]
    per = heads * STATE // wl.shape[1]
    total = dall.shape[0]
    vg_sum = [jnp.zeros((dl.shape[0], HEAD_DIM), F32) for _ in range(heads)]
    wg_sum = [jnp.zeros((dl.shape[0], STATE), F32) for _ in range(heads // per)]
    rg_sum = [jnp.zeros((dl.shape[0], STATE), F32) for _ in range(heads // per)]

    def dot_last(a, b):
        return lax.dot_general(a, b, LAST, preferred_element_type=F32)

    def step(i, carry):
        vg_sum, wg_sum, rg_sum = carry
        vg_sum, wg_sum, rg_sum = list(vg_sum), list(wg_sum), list(rg_sum)
        rows = pl.ds(pl.multiple_of(i * chunk, chunk), chunk)
        for g in range(heads // per):
            wide = slice(g * STATE, (g + 1) * STATE)
            read, write = rall[rows, wide], wall[rows, wide]
            common = dot_last(wl[:, wide], read)
            q1 = jnp.zeros((dl.shape[0], chunk), F32)
            q2 = jnp.zeros((dl.shape[0], chunk), F32)
            for h in range(g * per, (g + 1) * per):
                cols = slice(h * HEAD_DIM, (h + 1) * HEAD_DIM)
                delta, value = dall[rows, cols], vall[rows, cols]
                fade = jnp.exp(-jnp.abs(acol[:, h : h + 1] - arow[h : h + 1, rows]))
                vg_sum[h] += jnp.dot(
                    (fade * common).astype(BF16), delta, preferred_element_type=F32
                )
                q1 += fade * dot_last(vl[:, cols], delta)
                q2 += fade * dot_last(dl[:, cols], value)
            wg_sum[g] += jnp.dot(q1.astype(BF16), read, preferred_element_type=F32)
            rg_sum[g] += jnp.dot(q2.astype(BF16), write, preferred_element_type=F32)
        return tuple(vg_sum), tuple(wg_sum), tuple(rg_sum)

    vg_sum, wg_sum, rg_sum = lax.fori_loop(
        0, total // chunk, step, (tuple(vg_sum), tuple(wg_sum), tuple(rg_sum))
    )
    for h in range(heads):
        vg[:, h * HEAD_DIM : (h + 1) * HEAD_DIM] = vg_sum[h].astype(BF16)
    for g in range(heads // per):
        wg[:, g * STATE : (g + 1) * STATE] = wg_sum[g].astype(BF16)
        rg[:, g * STATE : (g + 1) * STATE] = rg_sum[g].astype(BF16)


def call(kernel, ident, ins, outs, scratch, operands, name):
    vm = pl.BlockSpec(memory_space=pltpu.VMEM)
    return pl.pallas_call(
        kernel,
        out_shape=outs,
        in_specs=[vm] * ins,
        out_specs=jax.tree.map(lambda _: vm, outs),
        scratch_shapes=scratch,
        compiler_params=pltpu.CompilerParams(
            collective_id=ident,
            has_side_effects=ident is not None,
            vmem_limit_bytes=56 * 1024 * 1024,
        ),
        cost_estimate=pl.CostEstimate(
            flops=4_000_000_000, bytes_accessed=8_000_000, transcendentals=0
        ),
        name=name,
    )(*operands)


def on_device(
    layer_input,
    cotangent,
    routes,
    route_weight,
    gate_weight,
    up_weight,
    down_weight,
    heads_value,
    output_gate,
    mixer_saved,
    proj_weight,
    state_write,
    state_read,
    decay_rate,
):
    n = lax.axis_size("sp")
    t = lax.axis_size("tp")
    me = lax.axis_index("sp")
    tokens, d = layer_input.shape
    top = routes.shape[1]
    capacity = max(2, 3 * tokens * top // (2 * n))
    slots_all = n * capacity
    sds = jax.ShapeDtypeStruct

    active_gate, slope_gate = silu_parts(output_gate.astype(F32))
    saved = mixer_saved.astype(F32)
    gated = (saved * active_gate).astype(BF16)

    flat = routes.reshape(-1)
    count = flat.shape[0]
    onehot = (flat[:, None] == jnp.arange(n, dtype=jnp.int32)[None, :]).astype(BF16)
    lower = (
        jnp.arange(count, dtype=jnp.int32)[:, None] > jnp.arange(count, dtype=jnp.int32)[None, :]
    ).astype(BF16)
    before = jnp.dot(lower, onehot, preferred_element_type=F32)
    ranks = jnp.sum(before * onehot.astype(F32), axis=1).astype(jnp.int32)
    slots = (flat * capacity + ranks).reshape(tokens, top)
    slot_ids = jnp.arange(slots_all, dtype=jnp.int32)
    hits = [(slots[:, k][None, :] == slot_ids[:, None]) for k in range(top)]
    pick = functools.reduce(jnp.logical_or, hits).astype(BF16)
    slot_weight = sum(
        jnp.sum(jnp.where(hits[k], route_weight[:, k][None, :], 0.0), axis=1) for k in range(top)
    )
    send_input = (
        jnp.dot(pick, layer_input, preferred_element_type=F32)
        .astype(BF16)
        .reshape(n, capacity, d)
    )
    send_cotangent = (
        (jnp.dot(pick, cotangent, preferred_element_type=F32) * slot_weight[:, None])
        .astype(BF16)
        .reshape(n, capacity, d)
    )
    decay_sum = jnp.cumsum(decay_rate, axis=0).T
    heads = decay_sum.shape[0]

    expert_input, expert_cotangent, decays = call(
        functools.partial(dispatch_kernel, n, t),
        1,
        3,
        (
            sds((n, capacity, t * d), BF16),
            sds((n, capacity, t * d), BF16),
            sds((n, heads, tokens), F32),
        ),
        [
            DMA((2, n)),
            DMA((2, n)),
            DMA((2, 3, n)),
            DMA((2, 3, n)),
            DMA((n,)),
            DMA((n,)),
            DMA((3,)),
        ],
        (send_input, send_cotangent, decay_sum),
        "dispatch",
    )
    expert_input = expert_input.reshape(slots_all, t * d)
    expert_cotangent = expert_cotangent.reshape(slots_all, t * d)
    gate_local = gate_weight[0]
    up_local = up_weight[0]
    down_local = down_weight[0]
    pre_gate = jnp.dot(expert_input, gate_local, preferred_element_type=F32)
    pre_up = jnp.dot(expert_input, up_local, preferred_element_type=F32)
    active, slope = silu_parts(pre_gate)
    hidden = (active * pre_up).astype(BF16)
    hidden_grad = lax.dot_general(expert_cotangent, down_local, LAST, preferred_element_type=F32)
    gate_delta = (hidden_grad * pre_up * slope).astype(BF16)
    up_delta = (hidden_grad * active).astype(BF16)
    partial_grad = lax.dot_general(gate_delta, gate_local, LAST, preferred_element_type=F32)
    partial_grad = partial_grad + lax.dot_general(
        up_delta, up_local, LAST, preferred_element_type=F32
    )
    partial_grad = partial_grad.astype(BF16).reshape(n, capacity, t * d)
    block = (n, capacity, d)
    arrived = call(
        functools.partial(combine_kernel, n, t),
        2,
        1,
        sds(block, BF16),
        [
            VMEM((2,) + block, BF16),
            VMEM(block, BF16),
            VMEM(block, BF16),
            VMEM(block, BF16),
            DMA((2,)),
            DMA((2,)),
            DMA((n,)),
            DMA((n,)),
            DMA((n,)),
            DMA((n,)),
            DMA((1,)),
        ],
        (partial_grad,),
        "combine",
    ).reshape(slots_all, d)
    moe_grad = lax.dot_general(pick, arrived, FIRST, preferred_element_type=F32)
    layer_grad = (cotangent.astype(F32) + moe_grad).astype(BF16)
    full_grad = call(
        functools.partial(rows_kernel, n, t),
        3,
        1,
        sds((tokens, t * d), BF16),
        [DMA((3,)), DMA((3,)), DMA((1,))],
        (layer_grad,),
        "rows",
    )
    out_delta = jnp.dot(full_grad, proj_weight, preferred_element_type=F32).astype(BF16)
    outgate_grad = (out_delta.astype(F32) * saved * slope_gate).astype(BF16)
    mixer_delta = (out_delta.astype(F32) * active_gate).astype(BF16)
    width = t * d // n
    by_owner = full_grad.reshape(tokens, n, width).transpose(1, 0, 2)
    length = max(1, n // 2)
    gathered = (mixer_delta, heads_value, gated, state_write, state_read)
    *gathered_all, all_grad = call(
        functools.partial(late_kernel, n, t),
        4,
        6,
        tuple(sds((n,) + x.shape, BF16) for x in gathered) + (sds((n, tokens, width), BF16),),
        [
            DMA((n,)),
            DMA((n,)),
            DMA((3, n)),
            DMA((3, n)),
            DMA((5,)),
            DMA((5,)),
            DMA((5, 2, 2, length)),
            DMA((5, 2, 2, length)),
            DMA((5, 2, length)),
            DMA((5, 2, length)),
            DMA((6,)),
        ],
        gathered + (by_owner,),
        "late",
    )
    all_delta, all_value, all_gated, all_write, all_read = (
        x.reshape(n * tokens, -1) for x in gathered_all
    )

    down_grad = lax.dot_general(hidden, expert_cotangent, FIRST, preferred_element_type=F32)
    gate_grad = lax.dot_general(expert_input, gate_delta, FIRST, preferred_element_type=F32)
    up_grad = lax.dot_general(expert_input, up_delta, FIRST, preferred_element_type=F32)

    state_w = state_write.shape[1]
    proj_grad = lax.dot_general(
        all_grad.reshape(n * tokens, width), all_gated, FIRST, preferred_element_type=F32
    )
    totals = decays[:, :, -1]
    start = jnp.cumsum(totals, axis=0) - totals
    decay_row = (decays + start[:, :, None]).transpose(1, 0, 2)
    decay_here = lax.dynamic_index_in_dim(decay_row, me, axis=1, keepdims=False).T
    chunk = min(4, n) * tokens
    value_grad, write_gradient, read_gradient = call(
        functools.partial(mixer_kernel, chunk),
        None,
        10,
        (sds((tokens, d), BF16), sds((tokens, state_w), BF16), sds((tokens, state_w), BF16)),
        [],
        (
            all_delta,
            all_value,
            all_read,
            all_write,
            decay_row.reshape(heads, n * tokens),
            decay_here,
            mixer_delta,
            heads_value,
            state_read,
            state_write,
        ),
        "mixer",
    )
    return (
        gate_grad.astype(BF16)[None],
        up_grad.astype(BF16)[None],
        down_grad.astype(BF16)[None],
        proj_grad,
        value_grad,
        write_gradient,
        read_gradient,
        outgate_grad,
    )


def solution(mesh):
    split = P("sp", "tp")
    in_specs = (
        split,
        split,
        P("sp", None),
        P("sp", None),
        P("sp", None, "tp"),
        P("sp", None, "tp"),
        P("sp", "tp", None),
        split,
        split,
        split,
        P(None, "tp"),
        split,
        split,
        split,
    )
    out_specs = (
        P("sp", None, "tp"),
        P("sp", None, "tp"),
        P("sp", "tp", None),
        split,
        split,
        split,
        split,
        split,
    )
    return jax.shard_map(
        on_device, mesh=mesh, in_specs=in_specs, out_specs=out_specs, check_vma=False
    )
```
